32 devices in a mesh: rep: 4 (over z), fs: 4 (over y, x), tp: 2 (over core).
Axes of the slice: x: 2, y: 2, z: 4, core: 2. Of those that a mesh axis runs over, the one named last changes fastest.
Arguments:
- residual: bfloat16 [16, 256, 2048], P(('rep', 'fs'), None, 'tp'), may hold values from -6 to 6
- queries: bfloat16 [16, 256, 2048], P(('rep', 'fs'), None, 'tp'), may hold values from -6 to 6
- key_matrix: bfloat16 [16, 256, 2048], P(('rep', 'fs'), None, 'tp'), may hold values from -6 to 6
- value_matrix: bfloat16 [16, 256, 2048], P(('rep', 'fs'), None, 'tp'), may hold values from -6 to 6
- decay_logodds: float32 [16, 256, 2048], P(('rep', 'fs'), None, 'tp'), may hold values from -3.4 to 8.9, as said below
- decay_surge: float32 [16, 256, 8], P(('rep', 'fs'), None, 'tp'), may hold values from -2.1 to 0, as said below
- head_norm_gain: float32 [256], replicated, may hold values from 0.1 to 1.9
- output_matrix: float32 [2048, 2048], P('fs', 'tp'), may hold values from -0.125 to 0.125
- output_column_scale: float32 [2048], P('tp'), may hold values from 0.5 to 2
- premix_norm_gain: float32 [2048], replicated, may hold values from 0.1 to 1.9
- gate_matrix: float32 [2048, 2816], P('fs', 'tp'), may hold values from -0.125 to 0.125
- gate_column_scale: float32 [2816], P('tp'), may hold values from 0.5 to 2
- up_matrix: float32 [2048, 2816], P('fs', 'tp'), may hold values from -0.125 to 0.125
- up_column_scale: float32 [2816], P('tp'), may hold values from 0.5 to 2
- down_matrix: float32 [2048, 2816], P('fs', 'tp'), may hold values from -0.109375 to 0.109375
- down_column_scale: float32 [2048], P('tp'), may hold values from 0.5 to 2
Outputs:
- layer_out: bfloat16 [16, 256, 2048], P(('rep', 'fs'), None, 'tp')
The draws below stay inside these ranges and needn't reach their ends.
Inputs may be any that keep to these rules, and one draw needn't show every extreme that they name: `decay_logodds`: log-odds of a key channel's decay. `decay_surge`: non-positive log-factors of a head's state.
All inputs are finite; a program needn't handle non-finite values.
Results may differ from the reference program's by a relative error of at most 0.018.
Values may be sent and summed in bfloat16 or wider, within the bound.
No kernel may reach another device: no remote copies, remote signals or barrier semaphores. Data moves between devices by JAX's collectives and lax.ppermute only.
A program may use at most 128 MiB of HBM per device.

```python
import math
import jax
import jax.numpy as jnp
from jax import lax

D = 2048
HEAD_NUMBER = 8
HEAD_V = 256
FF = 2816
BLOCK = 64
SEQUENCE_LENGTH = 256
KEY_DIM = 2048
VALUE_DIM = 2048
BATCH_SIZE = 16
N_TP = 2


def draw_decay_logodds(key, part):
    residual_flows = jax.random.split(jax.random.fold_in(key, 11), 5)
    slow_share = 0.5
    jitter = jnp.clip(0.7 * jax.random.normal(residual_flows[4], (BATCH_SIZE, SEQUENCE_LENGTH, KEY_DIM), jnp.float32), -2.8, 2.8)
    slow_mask = jax.random.uniform(residual_flows[0], (KEY_DIM,), jnp.float32) < slow_share
    slow_base = jax.random.uniform(residual_flows[1], (KEY_DIM,), jnp.float32, 3.5, 5.5)
    fast_base = jax.random.uniform(residual_flows[2], (KEY_DIM,), jnp.float32, 0.0, 1.2)
    offset = jax.random.uniform(residual_flows[3], (BATCH_SIZE, 1, 1), jnp.float32, -0.6, 0.6)
    return jnp.where(slow_mask, slow_base, fast_base) + offset + jitter


def draw_decay_surge(key, part):
    residual_flows = jax.random.split(jax.random.fold_in(key, 23), 2)
    surge_position = jax.random.randint(residual_flows[0], (BATCH_SIZE, 3, HEAD_NUMBER), 0, SEQUENCE_LENGTH)
    strength = jnp.log(jax.random.uniform(residual_flows[1], (BATCH_SIZE, 3, HEAD_NUMBER), jnp.float32, 0.5, 0.8))
    match_scores = jnp.arange(SEQUENCE_LENGTH)[None, :, None, None] == surge_position[:, None, :, :]
    return jnp.sum(jnp.where(match_scores, strength[:, None, :, :], 0.0), axis=2)


def block_levels(own_key, shape, cuts, low, top_value):
    def one(position, shards_of):
        draws = jax.random.uniform(jax.random.fold_in(jax.random.fold_in(own_key, 6), position), (shards_of,), jnp.float32, low / len(cuts), top_value / len(cuts))
        return jnp.repeat(jnp.exp(draws), shape[position] // shards_of).reshape((-1,) + (1,) * (len(shape) - position - 1))

    loudness = one(*cuts[0])
    for cut in cuts[1:]:
        loudness = loudness * one(*cut)
    return loudness


def gaussian(stream_key, dims, scale, bound, cuts=(), kind=jnp.bfloat16):
    values = jax.random.normal(stream_key, dims, jnp.float32) * scale
    if len(cuts) > 0:
        values = block_levels(stream_key, dims, cuts, -0.22, 0.18) * values
    return jnp.clip(values, min=-bound, max=bound).astype(kind)


def setup_inputs(seed: int = 0) -> dict:
    arg_keys = jax.random.split(jax.random.key(seed), 17)
    return {
        "residual": gaussian(arg_keys[0], (BATCH_SIZE, SEQUENCE_LENGTH, D), 1.0, 6.0, ((0, 16), (2, 2))),
        "queries": gaussian(arg_keys[1], (BATCH_SIZE, SEQUENCE_LENGTH, KEY_DIM), 1.0, 6.0, ((0, 16), (2, 2))),
        "key_matrix": gaussian(arg_keys[2], (BATCH_SIZE, SEQUENCE_LENGTH, KEY_DIM), 1.0, 6.0, ((0, 16), (2, 2))),
        "value_matrix": gaussian(arg_keys[3], (BATCH_SIZE, SEQUENCE_LENGTH, VALUE_DIM), 1.0, 6.0, ((0, 16), (2, 2))),
        "decay_logodds": draw_decay_logodds(jax.random.fold_in(arg_keys[16], 71), 0),
        "decay_surge": draw_decay_surge(jax.random.fold_in(arg_keys[16], 71), 0),
        "head_norm_gain": jnp.clip(1.0 + 0.18 * jax.random.normal(arg_keys[6], (HEAD_V,), jnp.float32), 0.1, 1.9),
        "output_matrix": gaussian(arg_keys[7], (D, VALUE_DIM), VALUE_DIM ** -0.5, 0.125, ((0, 4), (1, 2)), jnp.float32),
        "output_column_scale": jnp.clip(jnp.exp(math.log(2.0) - 1.3862944 * jax.random.uniform(arg_keys[8], (D,), jnp.float32) ** block_levels(arg_keys[8], (D,), ((0, 2),), -0.2, 0.2)), 0.5, 2.0),
        "premix_norm_gain": jnp.clip(1.0 + 0.18 * jax.random.normal(arg_keys[9], (D,), jnp.float32), 0.1, 1.9),
        "gate_matrix": gaussian(arg_keys[10], (D, FF), D ** -0.5, 0.125, ((0, 4), (1, 2)), jnp.float32),
        "gate_column_scale": jnp.clip(jnp.exp(math.log(2.0) - 1.3862944 * jax.random.uniform(arg_keys[11], (FF,), jnp.float32) ** block_levels(arg_keys[11], (FF,), ((0, 2),), -0.2, 0.2)), 0.5, 2.0),
        "up_matrix": gaussian(arg_keys[12], (D, FF), D ** -0.5, 0.125, ((0, 4), (1, 2)), jnp.float32),
        "up_column_scale": jnp.clip(jnp.exp(math.log(2.0) - 1.3862944 * jax.random.uniform(arg_keys[13], (FF,), jnp.float32) ** block_levels(arg_keys[13], (FF,), ((0, 2),), -0.2, 0.2)), 0.5, 2.0),
        "down_matrix": gaussian(arg_keys[14], (D, FF), FF ** -0.5, 0.109375, ((0, 4), (1, 2)), jnp.float32),
        "down_column_scale": jnp.clip(jnp.exp(math.log(2.0) - 1.3862944 * jax.random.uniform(arg_keys[15], (D,), jnp.float32) ** block_levels(arg_keys[15], (D,), ((0, 2),), -0.2, 0.2)), 0.5, 2.0),
    }


epsilon = 1e-06
softness_factor = 16.0
highest = lax.Precision.HIGHEST

def one_direction(query_heads, key_heads, value_heads, log_decay_values):
    sequence_batch, head_total, token_length, key_channel_width = query_heads.shape
    value_width = value_heads.shape[-1]
    block_count = token_length // BLOCK

    def blocks(tensor):
        return tensor.reshape(sequence_batch, head_total, block_count, BLOCK, tensor.shape[-1])
    q_blocks = blocks(query_heads)
    k_blocks = blocks(key_heads)
    v_blocks = blocks(value_heads)
    running = jnp.cumsum(blocks(log_decay_values), axis=3)
    block_end = running[:, :, :, -1:, :]
    q_dec = q_blocks * jnp.exp(running)
    k_inv = k_blocks * jnp.exp(-running)
    k_end = k_blocks * jnp.exp(block_end - running)
    lower_mask = jnp.tril(jnp.ones((BLOCK, BLOCK), jnp.float32))
    scores = jnp.einsum('shnid,shnjd->shnij', q_dec, k_inv, precision=highest) * lower_mask
    inner_part = jnp.einsum('shnij,shnje->shnie', scores, v_blocks, precision=highest)
    fading = jnp.exp(block_end[:, :, :, 0, :])

    def advance(memory, pieces):
        q_piece, k_piece, v_piece, f_piece = pieces
        carried = jnp.einsum('shcd,shde->shce', q_piece, memory, precision=highest)
        memory = f_piece[..., None] * memory + jnp.einsum('shcd,shce->shde', k_piece, v_piece, precision=highest)
        return (memory, carried)
    pieces = tuple((jnp.moveaxis(tensor, 2, 0) for tensor in (q_dec, k_end, v_blocks, fading)))
    initial = jnp.zeros((sequence_batch, head_total, key_channel_width, value_width), jnp.float32)
    _, carried = lax.scan(advance, initial, pieces)
    summed = inner_part + jnp.moveaxis(carried, 0, 2)
    return summed.reshape(sequence_batch, head_total, token_length, value_width)

def backwards(tensor):
    return tensor[:, :, ::-1]

def linear_attend(queries, key_matrix, value_matrix, decay_logodds, decay_surge, head_norm_gain):
    sequence_batch, token_length, head_total = decay_surge.shape
    key_channel_width = queries.shape[-1] // head_total
    value_width = value_matrix.shape[-1] // head_total

    def split_heads(tensor, width):
        return jnp.transpose(tensor.astype(jnp.float32).reshape(sequence_batch, token_length, head_total, width), (0, 2, 1, 3))
    query_heads = split_heads(queries, key_channel_width) * key_channel_width ** (-0.5)
    key_heads = split_heads(key_matrix, key_channel_width)
    value_heads = split_heads(value_matrix, value_width)
    gate_values = jax.nn.log_sigmoid(decay_logodds).reshape(sequence_batch, token_length, head_total, key_channel_width) / softness_factor
    log_decay_values = jnp.transpose(gate_values + decay_surge[..., None], (0, 2, 1, 3))
    forward = one_direction(query_heads, key_heads, value_heads, log_decay_values)
    backward = backwards(one_direction(backwards(query_heads), backwards(key_heads), backwards(value_heads), backwards(log_decay_values)))
    attended = forward + backward
    scaled = attended * lax.rsqrt(lax.optimization_barrier(jnp.mean(attended * attended, axis=-1, keepdims=True)) + epsilon) * head_norm_gain
    merged = jnp.transpose(scaled, (0, 2, 1, 3)).reshape(sequence_batch * token_length, head_total * value_width)
    return merged.astype(jnp.bfloat16)

def grouped(left, right):
    width = left.shape[1] // N_TP
    left_parts = left.reshape(left.shape[0], N_TP, width).astype(jnp.float32)
    right_parts = right.reshape(right.shape[0], N_TP, width).astype(jnp.float32)
    terms = jnp.einsum('lgc,dgc->gld', left_parts, right_parts, precision=highest)
    rounded = lax.optimization_barrier(terms.astype(jnp.bfloat16))
    return lax.optimization_barrier(jnp.sum(rounded.astype(jnp.float32), axis=0))

def rms_scaled(rows_in, gain):
    wide_rows = rows_in.astype(jnp.float32)
    factor = lax.rsqrt(lax.optimization_barrier(jnp.mean(wide_rows * wide_rows, axis=-1, keepdims=True)) + epsilon)
    return (wide_rows * factor * gain).astype(jnp.bfloat16)

def reference(residual, queries, key_matrix, value_matrix, decay_logodds, decay_surge, head_norm_gain, output_matrix, output_column_scale, premix_norm_gain, gate_matrix, gate_column_scale, up_matrix, up_column_scale, down_matrix, down_column_scale):
    out_half = output_matrix.astype(jnp.bfloat16)
    gate_half = gate_matrix.astype(jnp.bfloat16)
    up_half = up_matrix.astype(jnp.bfloat16)
    down_half = down_matrix.astype(jnp.bfloat16)

    def single_sequence(input_rows):
        residual_sequence, query_sequence, key_sequence, value_sequence, logodds_sequence, surge_sequence = input_rows
        normalized_rows = linear_attend(query_sequence[None], key_sequence[None], value_sequence[None], logodds_sequence[None], surge_sequence[None], head_norm_gain)
        mix_total = grouped(normalized_rows, out_half)
        updated = (residual_sequence.astype(jnp.float32) + output_column_scale * mix_total).astype(jnp.bfloat16)
        normin = rms_scaled(updated, premix_norm_gain)
        gate_pre = jnp.dot(normin, gate_half, preferred_element_type=jnp.float32) * gate_column_scale
        up_pre = jnp.dot(normin, up_half, preferred_element_type=jnp.float32) * up_column_scale
        hidden = (jax.nn.silu(gate_pre) * up_pre).astype(jnp.bfloat16)
        down_total = grouped(hidden, down_half)
        return (updated.astype(jnp.float32) + down_column_scale * down_total).astype(jnp.bfloat16)
    return lax.map(single_sequence, (residual, queries, key_matrix, value_matrix, decay_logodds, decay_surge))
```

```python
import functools

import jax
import jax.numpy as jnp
from jax import lax
from jax.experimental import pallas as pl
from jax.experimental.pallas import tpu as pltpu
from jax.sharding import PartitionSpec as P

BLOCK = 64

epsilon = 1e-06
softness_factor = 16.0
bf16 = jnp.bfloat16
f32 = jnp.float32


def attend_kernel(q_ref, k_ref, v_ref, odds_ref, surge_ref, gain_ref, out_ref):
    head = pl.program_id(1)
    tokens, width = q_ref.shape[1:]
    count = tokens // BLOCK
    surge_all = surge_ref[0]
    column = lax.broadcasted_iota(jnp.int32, surge_all.shape, 1)
    surge = jnp.sum(jnp.where(column == head, surge_all, 0.0), axis=1, keepdims=True)
    odds = odds_ref[0]
    log_decay = (jnp.minimum(odds, 0.0) - jnp.log1p(jnp.exp(-jnp.abs(odds)))) / softness_factor + surge
    row = lax.broadcasted_iota(jnp.int32, (BLOCK, BLOCK), 0)
    col = lax.broadcasted_iota(jnp.int32, (BLOCK, BLOCK), 1)
    lower = row >= col
    upper = row <= col
    tri = jnp.where(lower, 1.0, 0.0)

    def cut(tensor, n):
        return tensor[n * BLOCK : (n + 1) * BLOCK]

    query = q_ref[0].astype(f32) * width ** (-0.5)
    key = k_ref[0].astype(f32)
    value = v_ref[0]
    q_fwd, q_bwd, k_diag_f, k_diag_b, k_end, k_begin, total = [], [], [], [], [], [], []
    for n in range(count):
        step = cut(log_decay, n)
        running = lax.dot_general(
            tri, step, (((1,), (0,)), ((), ())), precision=lax.Precision.HIGHEST, preferred_element_type=f32
        )
        whole = running[BLOCK - 1 :, :]
        before = running - step
        after = whole - before
        q_n, k_n = cut(query, n), cut(key, n)
        q_fwd.append((q_n * jnp.exp(running)).astype(bf16))
        q_bwd.append((q_n * jnp.exp(after)).astype(bf16))
        k_diag_f.append((k_n * jnp.exp(-running)).astype(bf16))
        k_diag_b.append((k_n * jnp.exp(-after)).astype(bf16))
        k_end.append(k_n * jnp.exp(whole - running))
        k_begin.append(k_n * jnp.exp(before))
        total.append(jnp.exp(whole))

    def scores(left, right):
        return lax.dot_general(left, right, (((1,), (1,)), ((), ())), preferred_element_type=f32)

    gain = gain_ref[...]
    for n in range(count):
        fwd_keys, fade = [], None
        for m in range(n - 1, -1, -1):
            piece = k_end[m] if fade is None else k_end[m] * fade
            fwd_keys.insert(0, piece.astype(bf16))
            fade = total[m] if fade is None else fade * total[m]
        bwd_keys, fade = [], None
        for m in range(n + 1, count):
            piece = k_begin[m] if fade is None else k_begin[m] * fade
            bwd_keys.append(piece.astype(bf16))
            fade = total[m] if fade is None else fade * total[m]
        fwd = scores(q_fwd[n], jnp.concatenate(fwd_keys + [k_diag_f[n]], axis=0))
        bwd = scores(q_bwd[n], jnp.concatenate([k_diag_b[n]] + bwd_keys, axis=0))
        own = jnp.where(lower, fwd[:, n * BLOCK :], 0.0) + jnp.where(upper, bwd[:, :BLOCK], 0.0)
        pieces = []
        if n > 0:
            pieces.append(fwd[:, : n * BLOCK])
        pieces.append(own)
        if n < count - 1:
            pieces.append(bwd[:, BLOCK:])
        line = jnp.concatenate(pieces, axis=1).astype(bf16)
        attended = jnp.dot(line, value, preferred_element_type=f32)
        factor = lax.rsqrt(jnp.mean(attended * attended, axis=-1, keepdims=True) + epsilon)
        out_ref[0, n * BLOCK : (n + 1) * BLOCK, :] = (attended * factor * gain).astype(bf16)


def linear_attend(queries, key_matrix, value_matrix, decay_logodds, decay_surge, head_norm_gain):
    sequences, tokens, heads = decay_surge.shape
    key_width = queries.shape[-1] // heads
    value_width = value_matrix.shape[-1] // heads

    def spec(width):
        return pl.BlockSpec((1, tokens, width), lambda s, h: (s, 0, h))

    return pl.pallas_call(
        attend_kernel,
        grid=(sequences, heads),
        in_specs=[
            spec(key_width),
            spec(key_width),
            spec(value_width),
            spec(key_width),
            pl.BlockSpec((1, tokens, heads), lambda s, h: (s, 0, 0)),
            pl.BlockSpec((1, value_width), lambda s, h: (0, 0)),
        ],
        out_specs=spec(value_width),
        out_shape=jax.ShapeDtypeStruct((sequences, tokens, heads * value_width), bf16),
        compiler_params=pltpu.CompilerParams(dimension_semantics=("arbitrary", "arbitrary")),
        name="attend",
    )(queries, key_matrix, value_matrix, decay_logodds, decay_surge, head_norm_gain.reshape(1, -1))


def by_rows(left, right):
    return lax.dot_general(left, right, (((1,), (1,)), ((), ())), preferred_element_type=f32)


def body(
    residual,
    queries,
    key_matrix,
    value_matrix,
    decay_logodds,
    decay_surge,
    head_norm_gain,
    output_matrix,
    output_column_scale,
    premix_norm_gain,
    gate_matrix,
    gate_column_scale,
    up_matrix,
    up_column_scale,
    down_matrix,
    down_column_scale,
):
    sequence_batch, token_length, local_width = residual.shape
    row_count = sequence_batch * token_length
    members = lax.axis_size("rep")
    member = lax.axis_index("rep")
    units = gate_matrix.shape[1]
    share = units // members

    place = lax.broadcasted_iota(jnp.int32, (units, share), 0)
    wanted = lax.broadcasted_iota(jnp.int32, (units, share), 1) + member * share
    pick = (place == wanted).astype(bf16)

    def own_share(matrix):
        return jnp.dot(matrix.astype(bf16), pick, preferred_element_type=f32).astype(bf16)

    def own_scale(scale):
        return lax.dynamic_slice(scale, (member * share,), (share,))

    out_full = lax.all_gather(output_matrix.astype(bf16), "fs", axis=0, tiled=True)
    pair = jnp.concatenate([own_share(gate_matrix), own_share(up_matrix)], axis=1)
    pair_full = lax.all_gather(pair, "fs", axis=0, tiled=True)
    down_full = lax.all_gather(own_share(down_matrix), "fs", axis=0, tiled=True)

    normalized_rows = linear_attend(
        queries, key_matrix, value_matrix, decay_logodds, decay_surge, head_norm_gain
    ).reshape(row_count, -1)
    mix_terms = by_rows(normalized_rows, out_full)
    mix_total = lax.psum_scatter(
        mix_terms.astype(bf16), "tp", scatter_dimension=1, tiled=True
    ).astype(f32)
    own_rows = residual.reshape(row_count, local_width).astype(f32)
    updated = (own_rows + output_column_scale * mix_total).astype(bf16)
    group_rows = lax.all_gather(updated, "rep", axis=0, tiled=True)
    features = lax.all_gather(group_rows, "tp", axis=1, tiled=True)
    wide_rows = features.astype(f32)
    factor = lax.rsqrt(jnp.mean(wide_rows * wide_rows, axis=-1, keepdims=True) + epsilon)
    normin = (wide_rows * factor * premix_norm_gain).astype(bf16)
    both = jnp.dot(normin, pair_full, preferred_element_type=f32)
    gate_pre = both[:, :share] * own_scale(gate_column_scale)
    up_pre = both[:, share:] * own_scale(up_column_scale)
    hidden = (jax.nn.silu(gate_pre) * up_pre).astype(bf16)
    down_terms = by_rows(hidden, down_full).astype(bf16)
    down_half = lax.psum_scatter(down_terms, "tp", scatter_dimension=1, tiled=True)
    down_total = lax.psum_scatter(down_half, "rep", scatter_dimension=0, tiled=True).astype(f32)
    result = (updated.astype(f32) + down_column_scale * down_total).astype(bf16)
    return result.reshape(sequence_batch, token_length, local_width)


def solution(mesh):
    return jax.shard_map(
        body,
        mesh=mesh,
        in_specs=(
            P(("rep", "fs"), None, "tp"),
            P(("rep", "fs"), None, "tp"),
            P(("rep", "fs"), None, "tp"),
            P(("rep", "fs"), None, "tp"),
            P(("rep", "fs"), None, "tp"),
            P(("rep", "fs"), None, "tp"),
            P(),
            P("fs", "tp"),
            P("tp"),
            P(),
            P("fs", "tp"),
            P("tp"),
            P("fs", "tp"),
            P("tp"),
            P("fs", "tp"),
            P("tp"),
        ),
        out_specs=P(("rep", "fs"), None, "tp"),
        check_vma=False,
    )
```

```python
import functools

import jax
import jax.numpy as jnp
from jax import lax
from jax.experimental import pallas as pl
from jax.experimental.pallas import tpu as pltpu
from jax.sharding import PartitionSpec as P

BLOCK = 64

epsilon = 1e-06
softness_factor = 16.0
bf16 = jnp.bfloat16
f32 = jnp.float32


def attend_kernel(q_ref, k_ref, v_ref, odds_ref, surge_ref, gain_ref, out_ref):
    head = pl.program_id(1)
    tokens, width = q_ref.shape[1:]
    count = tokens // BLOCK
    surge_all = surge_ref[0]
    column = lax.broadcasted_iota(jnp.int32, surge_all.shape, 1)
    surge = jnp.sum(jnp.where(column == head, surge_all, 0.0), axis=1, keepdims=True)
    odds = odds_ref[0]
    log_decay = (jnp.minimum(odds, 0.0) - jnp.log1p(jnp.exp(-jnp.abs(odds)))) / softness_factor + surge
    row = lax.broadcasted_iota(jnp.int32, (BLOCK, BLOCK), 0)
    col = lax.broadcasted_iota(jnp.int32, (BLOCK, BLOCK), 1)
    lower = row >= col
    upper = row <= col
    tri = jnp.where(lower, 1.0, 0.0)

    def cut(tensor, n):
        return tensor[n * BLOCK : (n + 1) * BLOCK]

    query = q_ref[0].astype(f32) * width ** (-0.5)
    key = k_ref[0].astype(f32)
    value = v_ref[0]
    q_fwd, q_bwd, k_diag_f, k_diag_b, k_end, k_begin, total = [], [], [], [], [], [], []
    for n in range(count):
        step = cut(log_decay, n)
        running = lax.dot_general(
            tri, step, (((1,), (0,)), ((), ())), precision=lax.Precision.HIGHEST, preferred_element_type=f32
        )
        whole = running[BLOCK - 1 :, :]
        before = running - step
        after = whole - before
        q_n, k_n = cut(query, n), cut(key, n)
        q_fwd.append((q_n * jnp.exp(running)).astype(bf16))
        q_bwd.append((q_n * jnp.exp(after)).astype(bf16))
        k_diag_f.append((k_n * jnp.exp(-running)).astype(bf16))
        k_diag_b.append((k_n * jnp.exp(-after)).astype(bf16))
        k_end.append(k_n * jnp.exp(whole - running))
        k_begin.append(k_n * jnp.exp(before))
        total.append(jnp.exp(whole))

    def scores(left, right):
        return lax.dot_general(left, right, (((1,), (1,)), ((), ())), preferred_element_type=f32)

    gain = gain_ref[...]
    for n in range(count):
        fwd_keys, fade = [], None
        for m in range(n - 1, -1, -1):
            piece = k_end[m] if fade is None else k_end[m] * fade
            fwd_keys.insert(0, piece.astype(bf16))
            fade = total[m] if fade is None else fade * total[m]
        bwd_keys, fade = [], None
        for m in range(n + 1, count):
            piece = k_begin[m] if fade is None else k_begin[m] * fade
            bwd_keys.append(piece.astype(bf16))
            fade = total[m] if fade is None else fade * total[m]
        fwd = scores(q_fwd[n], jnp.concatenate(fwd_keys + [k_diag_f[n]], axis=0))
        bwd = scores(q_bwd[n], jnp.concatenate([k_diag_b[n]] + bwd_keys, axis=0))
        own = jnp.where(lower, fwd[:, n * BLOCK :], 0.0) + jnp.where(upper, bwd[:, :BLOCK], 0.0)
        pieces = []
        if n > 0:
            pieces.append(fwd[:, : n * BLOCK])
        pieces.append(own)
        if n < count - 1:
            pieces.append(bwd[:, BLOCK:])
        line = jnp.concatenate(pieces, axis=1).astype(bf16)
        attended = jnp.dot(line, value, preferred_element_type=f32)
        factor = lax.rsqrt(jnp.mean(attended * attended, axis=-1, keepdims=True) + epsilon)
        out_ref[0, n * BLOCK : (n + 1) * BLOCK, :] = (attended * factor * gain).astype(bf16)


def linear_attend(queries, key_matrix, value_matrix, decay_logodds, decay_surge, head_norm_gain):
    sequences, tokens, heads = decay_surge.shape
    key_width = queries.shape[-1] // heads
    value_width = value_matrix.shape[-1] // heads

    def spec(width):
        return pl.BlockSpec((1, tokens, width), lambda s, h: (s, 0, h))

    return pl.pallas_call(
        attend_kernel,
        grid=(sequences, heads),
        in_specs=[
            spec(key_width),
            spec(key_width),
            spec(value_width),
            spec(key_width),
            pl.BlockSpec((1, tokens, heads), lambda s, h: (s, 0, 0)),
            pl.BlockSpec((1, value_width), lambda s, h: (0, 0)),
        ],
        out_specs=spec(value_width),
        out_shape=jax.ShapeDtypeStruct((sequences, tokens, heads * value_width), bf16),
        compiler_params=pltpu.CompilerParams(dimension_semantics=("arbitrary", "arbitrary")),
        name="attend",
    )(queries, key_matrix, value_matrix, decay_logodds, decay_surge, head_norm_gain.reshape(1, -1))


def by_rows(left, right):
    return lax.dot_general(left, right, (((1,), (1,)), ((), ())), preferred_element_type=f32)


def shifted(tensor, axis, step):
    size = lax.axis_size(axis)
    return lax.ppermute(tensor, axis, [(i, (i + step) % size) for i in range(size)])


def crossed(tensor, axis, bit):
    return lax.ppermute(tensor, axis, [(i, i ^ bit) for i in range(lax.axis_size(axis))])


def after(tensor, *others):
    return lax.optimization_barrier((tensor,) + others)[0]


def gather_step(shard):
    return crossed(shard, "fs", 1), crossed(shard, "fs", 2)


def gather_finish(shard, near):
    half = shard.shape[0] // 2
    one, two = near
    far = jnp.concatenate([crossed(two[:half], "fs", 1), crossed(one[half:], "fs", 2)], axis=0)
    return [shard, one, two, far]


def in_order(pieces, start):
    rows = pieces[0].shape[0]
    total = rows * len(pieces)
    me = lax.axis_index("fs")
    full = jnp.zeros((total,) + pieces[0].shape[1:], pieces[0].dtype)
    for j, piece in enumerate(pieces):
        full = lax.dynamic_update_slice(full, piece, (((me ^ j) * rows - start) % total, 0))
    return full


def body(
    residual,
    queries,
    key_matrix,
    value_matrix,
    decay_logodds,
    decay_surge,
    head_norm_gain,
    output_matrix,
    output_column_scale,
    premix_norm_gain,
    gate_matrix,
    gate_column_scale,
    up_matrix,
    up_column_scale,
    down_matrix,
    down_column_scale,
):
    sequence_batch, token_length, local_width = residual.shape
    row_count = sequence_batch * token_length
    members = lax.axis_size("rep")
    member = lax.axis_index("rep")
    units = gate_matrix.shape[1]
    share = units // members
    paired = lax.axis_size("tp") == 2
    start = lax.axis_index("tp") * local_width if paired else 0

    place = lax.broadcasted_iota(jnp.int32, (units, share), 0)
    wanted = lax.broadcasted_iota(jnp.int32, (units, share), 1) + member * share
    pick = (place == wanted).astype(bf16)

    def own_share(matrix):
        return jnp.dot(matrix.astype(bf16), pick, preferred_element_type=f32).astype(bf16)

    def own_scale(scale):
        return lax.dynamic_slice(scale, (member * share,), (share,))

    out_half = output_matrix.astype(bf16)
    pair_half = jnp.concatenate([own_share(gate_matrix), own_share(up_matrix)], axis=1)
    down_half = own_share(down_matrix)
    if lax.axis_size("fs") == 4:
        out_near = gather_step(out_half)
        out_pieces = gather_finish(out_half, out_near)
        pair_half = after(pair_half, *out_near)
        pair_near = gather_step(pair_half)
        pair_pieces = gather_finish(pair_half, pair_near)
        down_half = after(down_half, *pair_near)
        down_pieces = gather_finish(down_half, gather_step(down_half))
        out_full, pair_full, down_full = (
            in_order(pieces, start) for pieces in (out_pieces, pair_pieces, down_pieces)
        )
    else:
        out_full, pair_full, down_full = (
            jnp.roll(lax.all_gather(half, "fs", axis=0, tiled=True), -start, axis=0)
            for half in (out_half, pair_half, down_half)
        )

    def product_over_tp(left, matrix):
        if not paired:
            terms = by_rows(left, matrix).astype(bf16)
            return lax.psum_scatter(terms, "tp", scatter_dimension=1, tiled=True).astype(f32)
        sent = by_rows(left, matrix[local_width:]).astype(bf16)
        arrived = crossed(sent, "tp", 1).astype(f32)
        return by_rows(left, matrix[:local_width]).astype(bf16).astype(f32) + arrived

    normalized_rows = linear_attend(
        queries, key_matrix, value_matrix, decay_logodds, decay_surge, head_norm_gain
    ).reshape(row_count, -1)
    mix_total = product_over_tp(normalized_rows, out_full)
    own_rows = residual.reshape(row_count, local_width).astype(f32)
    updated = (own_rows + output_column_scale * mix_total).astype(bf16)

    gain = jnp.roll(premix_norm_gain, -start)
    gate_scale, up_scale = own_scale(gate_column_scale), own_scale(up_column_scale)

    def mlp(rows):
        if paired:
            wide = jnp.concatenate([rows, crossed(rows, "tp", 1)], axis=1)
        else:
            wide = lax.all_gather(rows, "tp", axis=1, tiled=True)
        wide = wide.astype(f32)
        factor = lax.rsqrt(jnp.mean(wide * wide, axis=-1, keepdims=True) + epsilon)
        normin = (wide * factor * gain).astype(bf16)
        both = jnp.dot(normin, pair_full, preferred_element_type=f32)
        hidden = (jax.nn.silu(both[:, :share] * gate_scale) * (both[:, share:] * up_scale)).astype(bf16)
        return product_over_tp(hidden, down_full)

    half_rows = row_count // 2
    half_width = local_width // 2
    chunks = {0: updated}
    left, right = updated, updated
    for distance in range(1, members // 2 + 1):
        if 2 * distance == members:
            left, right = left[:half_rows], right[half_rows:]
            chunks[distance] = jnp.concatenate(
                [shifted(left, "rep", 1), shifted(right, "rep", -1)], axis=0
            )
        else:
            left, right = shifted(left, "rep", 1), shifted(right, "rep", -1)
            chunks[members - distance], chunks[distance] = left, right
    terms = {distance: mlp(chunks[distance]) for distance in sorted(chunks)}

    up_sum = down_sum = 0.0
    for step in range(members):
        up_sum = up_sum + terms[(members - 1 - step) % members][:, :half_width]
        down_sum = down_sum + terms[(1 + step) % members][:, half_width:]
        if step < members - 1:
            up_sum = shifted(up_sum.astype(bf16), "rep", 1).astype(f32)
            down_sum = shifted(down_sum.astype(bf16), "rep", -1).astype(f32)
    down_total = jnp.concatenate([up_sum, down_sum], axis=1)
    result = (updated.astype(f32) + down_column_scale * down_total).astype(bf16)
    return result.reshape(sequence_batch, token_length, local_width)


def solution(mesh):
    return jax.shard_map(
        body,
        mesh=mesh,
        in_specs=(
            P(("rep", "fs"), None, "tp"),
            P(("rep", "fs"), None, "tp"),
            P(("rep", "fs"), None, "tp"),
            P(("rep", "fs"), None, "tp"),
            P(("rep", "fs"), None, "tp"),
            P(("rep", "fs"), None, "tp"),
            P(),
            P("fs", "tp"),
            P("tp"),
            P(),
            P("fs", "tp"),
            P("tp"),
            P("fs", "tp"),
            P("tp"),
            P("fs", "tp"),
            P("tp"),
        ),
        out_specs=P(("rep", "fs"), None, "tp"),
        check_vma=False,
    )
```
